32 devices in a mesh: ep: 8 (over z, y), tp: 4 (over x, core).
Axes of the slice: x: 2, y: 2, z: 4, core: 2. Of those that a mesh axis runs over, the one named last changes fastest.
Arguments:
- tokens: bfloat16 [128, 1024], P('ep'), may hold values from -24 to 24
- seq_length: int32 [128], P('ep'), may hold values from 1024 to 16383
- ret_state: float32 [128, 4, 128, 256], P('ep', 'tp'), may hold values from -0.6 to 0.6
- norm_in: float32 [1024], replicated, may hold values from 0.1 to 1.9
- w_query: bfloat16 [1024, 512], P(None, 'tp'), may hold values from -0.1875 to 0.1875
- w_key: bfloat16 [1024, 512], P(None, 'tp'), may hold values from -0.1875 to 0.1875
- w_value: bfloat16 [1024, 1024], P(None, 'tp'), may hold values from -0.1875 to 0.1875
- head_gain: float32 [1024], P('tp'), may hold values from 0.1 to 1.9
- w_output: bfloat16 [1024, 1024], P('tp'), may hold values from -0.1875 to 0.1875
- norm_mid: float32 [1024], replicated, may hold values from 0.1 to 1.9
- route_expert: int32 [128, 2], P('ep'), may hold values from 0 to 3, all different within a row; in each aligned block of 16 rows (0 to 15, 16 to 31, ...) at most 12 rows name the same one
- route_score: float32 [128, 2], P('ep'), may hold values from -6 to 6
- expert_gate: bfloat16 [8, 1024, 1792], P('ep', None, 'tp'), may hold values from -0.1875 to 0.1875
- expert_up: bfloat16 [8, 1024, 1792], P('ep', None, 'tp'), may hold values from -0.1875 to 0.1875
- expert_down: bfloat16 [8, 1792, 1024], P('ep', 'tp'), may hold values from -0.09375 to 0.09375
Outputs:
- mixed: bfloat16 [128, 1024], P('ep', 'tp')
The draws below stay inside these ranges and needn't reach their ends.
Inputs may be any that keep to these rules, and one draw needn't show every extreme that they name: `route_expert`: each row names 2 different experts; within the rows of one device no expert is named by more than 12 rows, and some device's rows name one expert exactly 12 times.
All inputs are finite; a program needn't handle non-finite values.
Results may differ from the reference program's by a relative error of at most 0.014.
Values may be sent and summed in bfloat16 or wider, within the bound.
A program may use at most 64 MiB of HBM per device.

```python
import math
import jax
import jax.numpy as jnp
import numpy as np
from jax import lax

D = 1024
HEADS = 4
DK = 128
DV = 256
FF_E = 3584
SPREAD = 2
TOP_K = 2
SEQ_DEV = 16
BATCH = 128
EXPERTS = 4
CAP = 12
N_EP = 8
N_TP = 4


def draw_tokens(key, part):
    base_key, rough_key = jax.random.split(key, 2)
    column = jnp.arange(D, dtype=jnp.float32) / D
    column_ramp = jnp.exp(jnp.log(0.3) + jnp.log(10.0) * column)
    rough_scale = jax.random.uniform(rough_key, (D,), jnp.float32, 0.5, 1.5)
    base_draw = jnp.clip(jax.random.normal(base_key, (BATCH, D), jnp.float32), -5.0, 5.0)
    return (base_draw * column_ramp * rough_scale).astype(jnp.bfloat16)


def place_ends(array, key, low, largest):
    shape = array.shape
    place = [jax.random.randint(jax.random.fold_in(key, axis), (), 0, shape[axis]) for axis in range(len(shape))]
    array = array.at[tuple(place)].set(low)
    longest = shape.index(max(shape))
    place[longest] = (place[longest] + 1) % shape[longest]
    return array.at[tuple(place)].set(largest)


def block_scale(stream_key, dims, pieces, least, high):
    def one(dim, shards_of):
        steps = jax.random.uniform(jax.random.fold_in(jax.random.fold_in(stream_key, 6), dim), (shards_of,), jnp.float32, least / len(pieces), high / len(pieces))
        return jnp.repeat(jnp.exp(steps), dims[dim] // shards_of).reshape((-1,) + (1,) * (len(dims) - dim - 1))

    level = one(*pieces[0])
    for cut in pieces[1:]:
        level = level * one(*cut)
    return level


def assign_block(rng, own, number, rows, count, top, bound, slope):
    ranking = jax.random.permutation(rng, count)
    heavy_load, usual = shares(count, rows * top, bound, slope, True), shares(count, rows * top, bound, slope, False)
    places = jnp.arange(count)

    def named(lengths, turn):
        used = int((lengths > 0).sum())
        fixed = max(1, used // 4)
        shifted = fixed + (places - fixed + turn * (used - fixed)) % max(1, count - fixed)
        return jnp.zeros((count,), jnp.int32).at[ranking[jnp.where(places < fixed, places, shifted)]].set(jnp.asarray(lengths, jnp.int32))

    lengths = jnp.where(number % 4 == 0, named(heavy_load, number // 4), named(usual, number - number // 4 - 1))
    mixed = jax.random.permutation(jax.random.fold_in(own, 3), count)
    giver, taker = mixed[0:count // 2 * 2:2], mixed[1:count // 2 * 2:2]
    margin = jnp.minimum(lengths[giver] - 1, bound - lengths[taker]) // 2
    margin = jnp.where((giver == ranking[0]) | (taker == ranking[0]) | (lengths[taker] == 0), 0, jnp.maximum(margin, 0))
    shifted = jax.random.randint(jax.random.fold_in(own, 4), (count // 2,), 0, 1 << 20) % (margin + 1)
    lengths = lengths.at[giver].add(-shifted).at[taker].add(shifted)
    items = jnp.searchsorted(jnp.cumsum(lengths), jnp.arange(rows * top), side="right").astype(jnp.int32)
    listing = items.reshape(top, rows).T
    listing = listing[jax.random.permutation(jax.random.fold_in(own, 1), rows)]
    turn = jax.random.randint(jax.random.fold_in(own, 2), (rows, 1), 0, top)
    return jnp.take_along_axis(listing, (jnp.arange(top)[None, :] + turn) % top, axis=1)


def shares(number_of, total, reach, slope, full):
    loads = [(1 << 20) // math.isqrt(rank ** slope) + 1 for rank in range(1, number_of + 1)]
    largest = reach if full else min(reach, max(-(-total // number_of), total * loads[0] // sum(loads)))
    least = 1 if total - largest >= number_of - 1 else 0
    holding, surplus = [largest] + [least] * (number_of - 1), total - largest - least * (number_of - 1)
    while surplus > 0:
        movable = [i for i in range(1, number_of) if holding[i] < largest] or [i for i in range(1, number_of) if holding[i] < reach]
        mass, left = sum([loads[i] for i in movable]), surplus
        for i in movable:
            addition = min(reach - holding[i], max(1, left * loads[i] // mass), surplus)
            holding[i] = holding[i] + addition
            surplus = surplus - addition
    return np.array(holding)


def scatter_about(own_key, extent, width, bound, pieces=(), kind=jnp.bfloat16):
    values = jax.random.normal(own_key, extent, jnp.float32) * width
    if len(pieces) > 0:
        values = block_scale(own_key, extent, pieces, -0.22, 0.18) * values
    return jnp.clip(values, min=-bound, max=bound).astype(kind)


def setup_inputs(seed: int = 0) -> dict:
    splits = jax.random.split(jax.random.key(seed), 16)
    tokens = draw_tokens(jax.random.fold_in(splits[15], 71), 0)
    seq_length = place_ends(jax.random.randint(splits[1], (BATCH,), 1024, 16384), jax.random.fold_in(splits[1], 1), 1024, 16383).astype(jnp.int32)
    ret_state = scatter_about(splits[2], (BATCH, HEADS, DK, DV), 0.1, 0.6, ((0, 8), (1, 4)), jnp.float32)
    norm_in = jnp.clip(1.0 + 0.18 * jax.random.normal(splits[3], (D,), jnp.float32), 0.1, 1.9)
    w_query = scatter_about(splits[4], (D, HEADS * DK), D ** -0.5, 0.1875, ((1, 4),))
    w_key = scatter_about(splits[5], (D, HEADS * DK), D ** -0.5, 0.1875, ((1, 4),))
    w_value = scatter_about(splits[6], (D, HEADS * DV), D ** -0.5, 0.1875, ((1, 4),))
    head_gain = jnp.clip(1.0 + 0.18 * jax.random.normal(splits[7], (HEADS * DV,), jnp.float32), 0.1, 1.9)
    w_output = scatter_about(splits[8], (HEADS * DV, D), (HEADS * DV) ** -0.5, 0.1875, ((0, 4),))
    norm_mid = jnp.clip(1.0 + 0.18 * jax.random.normal(splits[9], (D,), jnp.float32), 0.1, 1.9)
    route_expert_keys = jax.random.split(jax.random.fold_in(splits[10], 1), BATCH // SEQ_DEV)
    route_expert_turns = jax.random.permutation(jax.random.fold_in(splits[10], 3), BATCH // SEQ_DEV)
    route_expert = jax.vmap(lambda own, number: assign_block(jax.random.fold_in(splits[10], 2), own, number, SEQ_DEV, EXPERTS, TOP_K, CAP, 2))(route_expert_keys, route_expert_turns).reshape((BATCH, TOP_K))
    route_score = scatter_about(splits[11], (BATCH, TOP_K), 1.5, 6.0, ((0, 8),), jnp.float32)
    expert_gate = scatter_about(splits[12], (EXPERTS * SPREAD, D, FF_E // SPREAD), D ** -0.5, 0.1875, ((0, 8), (2, 4)))
    expert_up = scatter_about(splits[13], (EXPERTS * SPREAD, D, FF_E // SPREAD), D ** -0.5, 0.1875, ((0, 8), (2, 4)))
    expert_down = scatter_about(splits[14], (EXPERTS * SPREAD, FF_E // SPREAD, D), FF_E ** -0.5, 0.09375, ((0, 8), (1, 4)))
    return dict(tokens=tokens, seq_length=seq_length, ret_state=ret_state, norm_in=norm_in, w_query=w_query, w_key=w_key, w_value=w_value, head_gain=head_gain, w_output=w_output, norm_mid=norm_mid, route_expert=route_expert, route_score=route_score, expert_gate=expert_gate, expert_up=expert_up, expert_down=expert_down)


EPS = 1e-06

def rotate(head_rows, positions):
    half_width = head_rows.shape[-1] // 2
    inverse = 10000.0 ** (-jnp.arange(half_width, dtype=jnp.float32) / half_width)
    angles = positions[:, None] * inverse[None, :]
    cosine = jnp.cos(angles)[:, None, :]
    sine_part = jnp.sin(angles)[:, None, :]
    first_half = head_rows[..., :half_width]
    second = head_rows[..., half_width:]
    return jnp.concatenate([first_half * cosine - second * sine_part, first_half * sine_part + second * cosine], axis=-1)

def expert_block(block_rows, gate_parts, up_parts, down_parts):
    results = []
    for part_index in range(SPREAD):
        gate_sum = jnp.dot(block_rows, gate_parts[part_index], preferred_element_type=jnp.float32)
        up_sum = jnp.dot(block_rows, up_parts[part_index], preferred_element_type=jnp.float32)
        hidden = (jax.nn.silu(gate_sum) * up_sum).astype(jnp.bfloat16)
        lane_width = hidden.shape[1] // N_TP
        totals = jnp.zeros((block_rows.shape[0], D), jnp.float32)
        for lane_index in range(N_TP):
            partial_value = jnp.dot(hidden[:, lane_index * lane_width:(lane_index + 1) * lane_width], down_parts[part_index, lane_index * lane_width:(lane_index + 1) * lane_width], preferred_element_type=jnp.float32).astype(jnp.bfloat16)
            totals = totals + lax.optimization_barrier(partial_value).astype(jnp.float32)
        results.append(totals.astype(jnp.bfloat16))
    return jnp.stack(results)

def reference(tokens, seq_length, ret_state, norm_in, w_query, w_key, w_value, head_gain, w_output, norm_mid, route_expert, route_score, expert_gate, expert_up, expert_down):
    token_f = tokens.astype(jnp.float32)
    normed = (token_f * lax.rsqrt(lax.optimization_barrier(jnp.mean(token_f * token_f, axis=-1, keepdims=True)) + EPS) * norm_in).astype(jnp.bfloat16)
    query_proj = jnp.dot(normed, w_query, preferred_element_type=jnp.float32).astype(jnp.bfloat16)
    key_proj = jnp.dot(normed, w_key, preferred_element_type=jnp.float32).astype(jnp.bfloat16)
    value_proj = jnp.dot(normed, w_value, preferred_element_type=jnp.float32).astype(jnp.bfloat16)
    positions = seq_length.astype(jnp.float32)
    q_rot = rotate(query_proj.astype(jnp.float32).reshape(BATCH, HEADS, DK), positions)
    k_rot = rotate(key_proj.astype(jnp.float32).reshape(BATCH, HEADS, DK), positions) * DK ** (-0.5)
    value_rows = value_proj.astype(jnp.float32).reshape(BATCH, HEADS, DV)
    decay_rate = 1.0 - jnp.exp2(-2.0 - 2.0 * jnp.arange(HEADS, dtype=jnp.float32))
    carried = jnp.einsum('bhd,bhde->bhe', q_rot, ret_state, precision=lax.Precision.HIGHEST)
    within = lax.optimization_barrier(jnp.sum(q_rot * k_rot, axis=-1, keepdims=True)) * value_rows
    retained = decay_rate[None, :, None] * carried + within
    centre = lax.optimization_barrier(jnp.mean(retained, axis=-1, keepdims=True))
    variance = lax.optimization_barrier(jnp.mean(jnp.square(retained - centre), axis=-1, keepdims=True))
    ret_out = ((retained - centre) * lax.rsqrt(variance + EPS)).reshape(BATCH, HEADS * DV)
    ret_out = (ret_out * head_gain).astype(jnp.bfloat16)
    span = HEADS * DV // N_TP
    attended = jnp.zeros((BATCH, D), jnp.float32)
    for lane_index in range(N_TP):
        partial_value = jnp.dot(ret_out[:, lane_index * span:(lane_index + 1) * span], w_output[lane_index * span:(lane_index + 1) * span], preferred_element_type=jnp.float32).astype(jnp.bfloat16)
        attended = attended + lax.optimization_barrier(partial_value).astype(jnp.float32)
    resid = (token_f + attended).astype(jnp.bfloat16)
    resid_f = resid.astype(jnp.float32)
    mid = (resid_f * lax.rsqrt(lax.optimization_barrier(jnp.mean(resid_f * resid_f, axis=-1, keepdims=True)) + EPS) * norm_mid).astype(jnp.bfloat16)
    flat_rows = route_expert.reshape(N_EP, SEQ_DEV * TOP_K)
    onehot = (flat_rows[..., None] == jnp.arange(EXPERTS, dtype=jnp.int32)[None, None, :]).astype(jnp.int32)
    rank_index = lax.optimization_barrier(jnp.sum((jnp.cumsum(onehot, axis=1) - onehot) * onehot, axis=2)).astype(jnp.int32)
    slot_index = (jnp.arange(N_EP, dtype=jnp.int32)[:, None] * CAP + rank_index).reshape(-1)
    token_index = (jnp.arange(BATCH * TOP_K, dtype=jnp.int32) // TOP_K).astype(jnp.int32)
    expert_index = flat_rows.reshape(-1)
    buffer = jnp.zeros((EXPERTS, N_EP * CAP, D), jnp.bfloat16).at[expert_index, slot_index].set(mid[token_index])
    gate_parts = expert_gate.reshape(EXPERTS, SPREAD, D, FF_E // SPREAD)
    up_parts = expert_up.reshape(EXPERTS, SPREAD, D, FF_E // SPREAD)
    down_parts = expert_down.reshape(EXPERTS, SPREAD, FF_E // SPREAD, D)
    results = lax.map(lambda packed: expert_block(packed[0], packed[1], packed[2], packed[3]), (buffer, gate_parts, up_parts, down_parts))
    picked = results[expert_index, :, slot_index, :]
    summed = lax.optimization_barrier(jnp.sum(picked.astype(jnp.float32), axis=1)).astype(jnp.bfloat16)
    summed = lax.optimization_barrier(summed).astype(jnp.float32).reshape(BATCH, TOP_K, D)
    weights = jax.nn.softmax(route_score, axis=-1)
    expert_mix = lax.optimization_barrier(jnp.sum(weights[..., None] * summed, axis=1))
    return (resid_f + expert_mix).astype(jnp.bfloat16)
```

```python
import functools

import jax
import jax.numpy as jnp
import numpy as np
from jax import lax
from jax.experimental import pallas as pl
from jax.experimental.pallas import tpu as pltpu
from jax.sharding import PartitionSpec as P

DK = 128
DV = 256
SPREAD = 2
CORES = 2
EPS = 1e-06
F32 = jnp.float32
BF16 = jnp.bfloat16


def each(low, high, step):
    if high - low <= 8:
        for index in range(low, high):
            step(index)
    else:

        def one(index, carry):
            step(index)
            return carry

        lax.fori_loop(low, high, one, 0)


def dot_rows(left, right):
    return lax.dot_general(left, right, (((1,), (1,)), ((), ())), preferred_element_type=F32)


def sin_cos(angles):
    turns = jnp.floor(angles * np.float32(2.0 / np.pi) + 0.5)
    rest = angles - turns * np.float32(1.5703125)
    rest = rest - turns * np.float32(4.837512969970703125e-4)
    rest = rest - turns * np.float32(7.54978995489188216e-8)
    square = rest * rest
    sine = rest + rest * square * (
        -1.6666654611e-1 + square * (8.3321608736e-3 - square * 1.9515295891e-4)
    )
    cosine = 1.0 - 0.5 * square + square * square * (
        4.166664568298827e-2 + square * (-1.388731625493765e-3 + square * 2.443315711809948e-5)
    )
    quarter = turns - 4.0 * jnp.floor(turns * 0.25)
    odd = (quarter == 1.0) | (quarter == 3.0)
    sin_base = jnp.where(odd, cosine, sine)
    cos_base = jnp.where(odd, sine, cosine)
    sin_value = jnp.where(quarter >= 2.0, -sin_base, sin_base)
    cos_value = jnp.where((quarter == 1.0) | (quarter == 2.0), -cos_base, cos_base)
    return sin_value, cos_value


def kernel(
    n_ep,
    n_tp,
    tokens,
    seq_length,
    inverse,
    norm_in,
    head_gain,
    norm_mid,
    route_expert,
    route_score,
    state_hbm,
    wq_hbm,
    wk_hbm,
    wv_hbm,
    wo_hbm,
    gate_hbm,
    up_hbm,
    down_hbm,
    out,
    state,
    wq,
    wk,
    wv,
    wo,
    gate,
    up,
    down,
    carried,
    part,
    part_in,
    resid,
    rows,
    hidden,
    pair_out,
    pair_in,
    own_sum,
    share,
    arrived,
    load_sem,
    tp_send,
    tp_recv,
    row_send,
    row_recv,
    fwd_send,
    fwd_recv,
    pair_send,
    pair_recv,
    ret_send,
    ret_recv,
):
    n_x = n_tp // CORES
    e = lax.axis_index("ep")
    t = lax.axis_index("tp")
    x = t // CORES
    c = t % CORES
    sibling = x * CORES + 1 - c
    n_rows = tokens.shape[0]
    width = tokens.shape[1]
    half = width // CORES
    quarter = width // n_tp
    heads = wq.shape[1] // DK
    n_state = 4 if n_rows % 4 == 0 else 1
    per = n_rows // n_state

    def to(ep_index, tp_index):
        return (ep_index, tp_index)

    barrier = pltpu.get_barrier_semaphore()

    def greet(d):
        for dx in range(n_x):
            peer = to((e + d) % n_ep, ((x + dx) % n_x) * CORES + c)
            pl.semaphore_signal(
                barrier, inc=1, device_id=peer, device_id_type=pl.DeviceIdType.MESH
            )

    loads = []
    pairs = [(wq_hbm, wq), (wk_hbm, wk), (wv_hbm, wv)]
    for i in range(n_state):
        pairs.append((state_hbm.at[pl.ds(i * per, per)], state.at[pl.ds(i * per, per)]))
    pairs += [
        (wo_hbm, wo),
        (gate_hbm.at[0], gate),
        (up_hbm.at[0], up),
        (down_hbm.at[0], down),
    ]
    for i, (source, target) in enumerate(pairs):
        load = pltpu.make_async_copy(source, target, load_sem.at[i])
        load.start()
        loads.append(load)
    for dx in range(1, n_x):
        peer = to(e, ((x + dx) % n_x) * CORES + c)
        pl.semaphore_signal(barrier, inc=1, device_id=peer, device_id_type=pl.DeviceIdType.MESH)
    for dx in range(n_x):
        peer = to(e, ((x + dx) % n_x) * CORES + 1 - c)
        pl.semaphore_signal(barrier, inc=1, device_id=peer, device_id_type=pl.DeviceIdType.MESH)
    each(1, n_ep, greet)

    token_f = tokens[...].astype(F32)
    scale = lax.rsqrt(jnp.mean(token_f * token_f, axis=-1, keepdims=True) + EPS)
    normed = (token_f * scale * norm_in[...]).astype(BF16)
    eye = lax.broadcasted_iota(jnp.int32, (n_rows, n_rows), 0) == lax.broadcasted_iota(
        jnp.int32, (n_rows, n_rows), 1
    )

    def column(row):
        return jnp.sum(jnp.where(eye, row, 0.0), axis=-1, keepdims=True)

    positions = column(seq_length[...].astype(F32))
    sine, cosine = sin_cos(positions * inverse[...])
    low_half = lax.broadcasted_iota(jnp.int32, (n_rows, DK), 1) < DK // 2
    sine = jnp.where(low_half, -sine, sine)
    score = route_score[...]
    raised = jnp.exp(score - jnp.max(score, axis=0, keepdims=True))
    softmax = raised / jnp.sum(raised, axis=0, keepdims=True)

    top_k = route_expert.shape[0]
    chosen = [column(route_expert[j : j + 1, :].astype(F32)) for j in range(top_k)]
    weights = [column(softmax[j : j + 1, :]) for j in range(top_k)]

    loads[0].wait()
    query = jnp.dot(normed, wq[...], preferred_element_type=F32).astype(BF16).astype(F32)
    loads[1].wait()
    key = jnp.dot(normed, wk[...], preferred_element_type=F32).astype(BF16).astype(F32)
    loads[2].wait()
    value = jnp.dot(normed, wv[...], preferred_element_type=F32).astype(BF16).astype(F32)

    for h in range(heads):
        q = query[:, h * DK : (h + 1) * DK]
        k = key[:, h * DK : (h + 1) * DK]
        v = value[:, h * DV : (h + 1) * DV]
        q = q * cosine + pltpu.roll(q, DK // 2, 1) * sine
        k = (k * cosine + pltpu.roll(k, DK // 2, 1) * sine) * np.float32(DK**-0.5)
        within = jnp.sum(q * k, axis=-1, keepdims=True) * v
        turned = q.T
        for b in range(n_rows):
            if h == 0 and b % per == 0:
                loads[3 + b // per].wait()
            carried[b : b + 1, :] = jnp.sum(
                turned[:, b : b + 1] * state[b, h], axis=0, keepdims=True
            )
        head = jnp.broadcast_to(t * heads + h, (1, 1)).astype(F32)
        decay = 1.0 - jnp.exp2(-2.0 - 2.0 * head)
        retained = decay * carried[...] + within
        centred = retained - jnp.mean(retained, axis=-1, keepdims=True)
        variance = jnp.mean(centred * centred, axis=-1, keepdims=True)
        normal = (
            centred * lax.rsqrt(variance + EPS) * head_gain[:, h * DV : (h + 1) * DV]
        ).astype(BF16)
        if h == 0:
            loads[3 + n_state].wait()
        product = jnp.dot(normal, wo[h * DV : (h + 1) * DV, :], preferred_element_type=F32)
        attended = product if h == 0 else attended + product
    attended = attended.astype(BF16)
    part[...] = attended

    pl.semaphore_wait(barrier, greetings(n_ep, n_x))

    sends = []
    for d in range(1, n_tp):
        copy = pltpu.make_async_remote_copy(
            src_ref=part,
            dst_ref=part_in.at[d - 1],
            send_sem=tp_send.at[d - 1],
            recv_sem=tp_recv.at[d - 1],
            device_id=to(e, (t + d) % n_tp),
            device_id_type=pl.DeviceIdType.MESH,
        )
        copy.start()
        sends.append(copy)
    total = attended.astype(F32)
    for copy in sends:
        copy.wait_recv()
    for d in range(1, n_tp):
        total = total + part_in[d - 1].astype(F32)
    resid_f = (token_f + total).astype(BF16).astype(F32)
    resid[...] = resid_f
    scale = lax.rsqrt(jnp.mean(resid_f * resid_f, axis=-1, keepdims=True) + EPS)
    mid = (resid_f * scale * norm_mid[...]).astype(BF16)
    for j in range(CORES):
        rows[e, j] = mid[:, j * half : (j + 1) * half]

    def row_copy(d):
        return pltpu.make_async_remote_copy(
            src_ref=rows.at[e, c],
            dst_ref=rows.at[e, c],
            send_sem=row_send.at[d],
            recv_sem=row_recv.at[d],
            device_id=to((e + d) % n_ep, t),
            device_id_type=pl.DeviceIdType.MESH,
        )

    def row_arrival(d):
        origin = (e + n_ep - d) % n_ep
        return pltpu.make_async_remote_copy(
            src_ref=rows.at[origin, c],
            dst_ref=rows.at[origin, c],
            send_sem=row_send.at[d],
            recv_sem=row_recv.at[d],
            device_id=to((e + d) % n_ep, t),
            device_id_type=pl.DeviceIdType.MESH,
        )

    def forward(d, lane):
        origin = (e + n_ep - d) % n_ep
        return pltpu.make_async_remote_copy(
            src_ref=rows.at[origin, lane],
            dst_ref=rows.at[origin, lane],
            send_sem=fwd_send.at[d],
            recv_sem=fwd_recv.at[d],
            device_id=to(e, sibling),
            device_id_type=pl.DeviceIdType.MESH,
        )

    each(1, n_ep, lambda d: row_copy(d).start())

    def relay(d):
        row_arrival(d).wait_recv()
        forward(d, c).start()

    each(1, n_ep, relay)
    each(1, n_ep, lambda d: forward(d, 1 - c).wait_recv())
    for copy in loads[4 + n_state :]:
        copy.wait()

    group = 8 if n_ep % 8 == 0 else n_ep
    span = group * n_rows

    def expert(i):
        block = rows[pl.ds(i * group, group)]
        gate_sum = jnp.zeros((span, gate.shape[0]), F32)
        up_sum = jnp.zeros((span, gate.shape[0]), F32)
        for j in range(CORES):
            piece = block[:, j].reshape(span, half)
            gate_sum += dot_rows(piece, gate[:, j * half : (j + 1) * half])
            up_sum += dot_rows(piece, up[:, j * half : (j + 1) * half])
        hidden[pl.ds(i * span, span), :] = (jax.nn.silu(gate_sum) * up_sum).astype(BF16)

    each(0, n_ep // group, expert)

    def columns(i, j, core):
        start = pl.multiple_of((j * CORES + core) * quarter, quarter)
        return jnp.dot(
            hidden[pl.ds(i * span, span), :],
            down[:, pl.ds(start, quarter)],
            preferred_element_type=F32,
        )

    pair_copies = []
    for j in range(n_x):

        def other(i, j=j):
            pair_out[j, pl.ds(i * group, group)] = (
                columns(i, j, 1 - c).astype(BF16).reshape(group, n_rows, quarter)
            )

        each(0, n_ep // group, other)
        copy = pltpu.make_async_remote_copy(
            src_ref=pair_out.at[j],
            dst_ref=pair_in.at[j],
            send_sem=pair_send.at[j],
            recv_sem=pair_recv.at[j],
            device_id=to(e, sibling),
            device_id_type=pl.DeviceIdType.MESH,
        )
        copy.start()
        pair_copies.append(copy)

    def return_copy(d, dx):
        target = (e + d) % n_ep
        lane = (x + dx) % n_x
        return pltpu.make_async_remote_copy(
            src_ref=share.at[lane, target],
            dst_ref=arrived.at[dx, d],
            send_sem=ret_send.at[dx, d],
            recv_sem=ret_recv.at[dx, d],
            device_id=to(target, lane * CORES + c),
            device_id_type=pl.DeviceIdType.MESH,
        )

    for dx in range(n_x):

        def own(i, dx=dx):
            mine = columns(i, (x + dx) % n_x, c)
            own_sum[dx, pl.ds(i * group, group)] = mine.reshape(group, n_rows, quarter)

        each(0, n_ep // group, own)
    for copy in pair_copies:
        copy.wait_recv()
    for dx in [*range(1, n_x), 0]:
        lane = (x + dx) % n_x

        def add(i, dx=dx, lane=lane):
            here = pl.ds(i * group, group)
            share[lane, here] = (own_sum[dx, here] + pair_in[lane, here].astype(F32)).astype(BF16)

        each(0, n_ep // group, add)
        each(0 if dx else 1, n_ep, lambda d, dx=dx: return_copy(d, dx).start())

    def mixing(d):
        expert_index = ((e + n_ep - d) % n_ep) // SPREAD
        wanted = jnp.broadcast_to(expert_index, (1, 1)).astype(F32)
        total = jnp.where(chosen[0] == wanted, weights[0], 0.0)
        for j in range(1, top_k):
            total = total + jnp.where(chosen[j] == wanted, weights[j], 0.0)
        return total

    start = pl.multiple_of(t * quarter, quarter)
    out_sum = resid[:, pl.ds(start, quarter)] + mixing(0) * share[x, e].astype(F32)
    if n_ep <= 8:
        for dx in [0, *range(1, n_x)]:
            for d in range(0 if dx else 1, n_ep):
                return_copy(d, dx).wait_recv()
                out_sum = out_sum + mixing(d) * arrived[dx, d].astype(F32)
    else:
        for dx in range(n_x):

            def gather(d, carry, dx=dx):
                return_copy(d, dx).wait_recv()
                return carry + mixing(d) * arrived[dx, d].astype(F32)

            out_sum = lax.fori_loop(0 if dx else 1, n_ep, gather, out_sum)
    out[...] = out_sum.astype(BF16)

    for copy in sends + pair_copies:
        copy.wait_send()

    def finish(d):
        row_copy(d).wait_send()
        forward(d, c).wait_send()
        return_copy(d, 0).wait_send()

    each(1, n_ep, finish)
    for dx in range(1, n_x):
        each(0, n_ep, lambda d, dx=dx: return_copy(d, dx).wait_send())


def greetings(n_ep, n_x):
    return n_x * (n_ep - 1) + (n_x - 1) + n_x


def body(
    n_ep,
    n_tp,
    tokens,
    seq_length,
    ret_state,
    norm_in,
    w_query,
    w_key,
    w_value,
    head_gain,
    w_output,
    norm_mid,
    route_expert,
    route_score,
    expert_gate,
    expert_up,
    expert_down,
):
    n_rows, width = tokens.shape
    quarter = width // n_tp
    half = width // CORES
    n_x = n_tp // CORES
    hidden_units = expert_gate.shape[2]
    angle = np.arange(DK, dtype=np.float64) % (DK // 2)
    inverse = jnp.asarray((10000.0 ** (-angle / (DK // 2))).astype(np.float32)[None, :])
    vmem = pl.BlockSpec(memory_space=pltpu.VMEM)
    anywhere = pl.BlockSpec(memory_space=pl.ANY)
    dma = pltpu.SemaphoreType.DMA
    return pl.pallas_call(
        functools.partial(kernel, n_ep, n_tp),
        out_shape=jax.ShapeDtypeStruct((n_rows, quarter), BF16),
        in_specs=[vmem] * 8 + [anywhere] * 8,
        out_specs=vmem,
        scratch_shapes=[
            pltpu.VMEM(ret_state.shape, F32),
            pltpu.VMEM(w_query.shape, BF16),
            pltpu.VMEM(w_key.shape, BF16),
            pltpu.VMEM(w_value.shape, BF16),
            pltpu.VMEM(w_output.shape, BF16),
            pltpu.VMEM((hidden_units, width), BF16),
            pltpu.VMEM((hidden_units, width), BF16),
            pltpu.VMEM(expert_down.shape[1:], BF16),
            pltpu.VMEM((n_rows, DV), F32),
            pltpu.VMEM((n_rows, width), BF16),
            pltpu.VMEM((n_tp - 1, n_rows, width), BF16),
            pltpu.VMEM((n_rows, width), F32),
            pltpu.VMEM((n_ep, CORES, n_rows, half), BF16),
            pltpu.VMEM((n_ep * n_rows, hidden_units), BF16),
            pltpu.VMEM((n_x, n_ep, n_rows, quarter), BF16),
            pltpu.VMEM((n_x, n_ep, n_rows, quarter), BF16),
            pltpu.VMEM((n_x, n_ep, n_rows, quarter), F32),
            pltpu.VMEM((n_x, n_ep, n_rows, quarter), BF16),
            pltpu.VMEM((n_x, n_ep, n_rows, quarter), BF16),
            dma((12,)),
            dma((n_tp - 1,)),
            dma((n_tp - 1,)),
            dma((n_ep,)),
            dma((n_ep,)),
            dma((n_ep,)),
            dma((n_ep,)),
            dma((n_x,)),
            dma((n_x,)),
            dma((n_x, n_ep)),
            dma((n_x, n_ep)),
        ],
        compiler_params=pltpu.CompilerParams(collective_id=0, has_side_effects=True),
    )(
        tokens,
        seq_length.reshape(1, n_rows),
        inverse,
        norm_in.reshape(1, width),
        head_gain.reshape(1, -1),
        norm_mid.reshape(1, width),
        route_expert.T,
        route_score.T,
        ret_state,
        w_query,
        w_key,
        w_value,
        w_output,
        jnp.swapaxes(expert_gate, 1, 2),
        jnp.swapaxes(expert_up, 1, 2),
        expert_down,
    )


def solution(mesh):
    placed = (
        P("ep", None),
        P("ep"),
        P("ep", "tp", None, None),
        P(),
        P(None, "tp"),
        P(None, "tp"),
        P(None, "tp"),
        P("tp"),
        P("tp", None),
        P(),
        P("ep", None),
        P("ep", None),
        P("ep", None, "tp"),
        P("ep", None, "tp"),
        P("ep", "tp", None),
    )
    step = functools.partial(body, mesh.shape["ep"], mesh.shape["tp"])
    return jax.shard_map(step, mesh=mesh, in_specs=placed, out_specs=P("ep", "tp"), check_vma=False)
```

```python
import functools

import jax
import jax.numpy as jnp
import numpy as np
from jax import lax
from jax.experimental import pallas as pl
from jax.experimental.pallas import tpu as pltpu
from jax.sharding import PartitionSpec as P

DK = 128
DV = 256
SPREAD = 2
CORES = 2
EPS = 1e-06
F32 = jnp.float32
BF16 = jnp.bfloat16


def each(low, high, step):
    if high - low <= 8:
        for index in range(low, high):
            step(index)
    else:

        def one(index, carry):
            step(index)
            return carry

        lax.fori_loop(low, high, one, 0)


def dot_rows(left, right):
    return lax.dot_general(left, right, (((1,), (1,)), ((), ())), preferred_element_type=F32)


def sin_cos(angles):
    turns = jnp.floor(angles * np.float32(2.0 / np.pi) + 0.5)
    rest = angles - turns * np.float32(1.5703125)
    rest = rest - turns * np.float32(4.837512969970703125e-4)
    rest = rest - turns * np.float32(7.54978995489188216e-8)
    square = rest * rest
    sine = rest + rest * square * (
        -1.6666654611e-1 + square * (8.3321608736e-3 - square * 1.9515295891e-4)
    )
    cosine = 1.0 - 0.5 * square + square * square * (
        4.166664568298827e-2 + square * (-1.388731625493765e-3 + square * 2.443315711809948e-5)
    )
    quarter = turns - 4.0 * jnp.floor(turns * 0.25)
    odd = (quarter == 1.0) | (quarter == 3.0)
    sin_base = jnp.where(odd, cosine, sine)
    cos_base = jnp.where(odd, sine, cosine)
    sin_value = jnp.where(quarter >= 2.0, -sin_base, sin_base)
    cos_value = jnp.where((quarter == 1.0) | (quarter == 2.0), -cos_base, cos_base)
    return sin_value, cos_value


def kernel(
    n_ep,
    n_tp,
    tokens,
    seq_length,
    inverse,
    norm_in,
    head_gain,
    norm_mid,
    route_expert,
    route_score,
    state_hbm,
    wq_hbm,
    wk_hbm,
    wv_hbm,
    wo_hbm,
    gate_hbm,
    up_hbm,
    down_hbm,
    out,
    state,
    wq,
    wk,
    wv,
    wo,
    gate,
    up,
    down,
    carried,
    part,
    part_in,
    resid,
    rows,
    hidden,
    pair_out,
    pair_in,
    own_sum,
    share,
    arrived,
    round_sem,
    ready_sem,
    load_sem,
    tp_send,
    tp_recv,
    row_send,
    row_recv,
    fwd_send,
    fwd_recv,
    pair_send,
    pair_recv,
    ret_send,
    ret_recv,
):
    n_x = n_tp // CORES
    e = lax.axis_index("ep")
    t = lax.axis_index("tp")
    x = t // CORES
    c = t % CORES
    sibling = x * CORES + 1 - c
    n_rows = tokens.shape[0]
    width = tokens.shape[1]
    half = width // CORES
    quarter = width // n_tp
    heads = wq.shape[1] // DK
    n_state = 4 if n_rows % 4 == 0 else 1
    per = n_rows // n_state

    def to(ep_index, tp_index):
        return (ep_index, tp_index)

    barrier = pltpu.get_barrier_semaphore()

    def signal(semaphore, peer):
        pl.semaphore_signal(
            semaphore, inc=1, device_id=peer, device_id_type=pl.DeviceIdType.MESH
        )

    powers = [1 << i for i in range(n_ep.bit_length() - 1)]
    cube = [to(e + w * (1 - 2 * ((e // w) % 2)), t) for w in powers]
    for d in range(1, n_tp):
        signal(barrier, to(e, (t + d) % n_tp))
    for peer in cube:
        signal(barrier, peer)
    loads = []
    pairs = [(wq_hbm, wq), (wk_hbm, wk), (wv_hbm, wv)]
    for i in range(n_state):
        pairs.append((state_hbm.at[pl.ds(i * per, per)], state.at[pl.ds(i * per, per)]))
    pairs += [
        (wo_hbm, wo),
        (gate_hbm.at[0], gate),
        (up_hbm.at[0], up),
        (down_hbm.at[0], down),
    ]
    for i, (source, target) in enumerate(pairs):
        load = pltpu.make_async_copy(source, target, load_sem.at[i])
        load.start()
        loads.append(load)
    token_f = tokens[...].astype(F32)
    scale = lax.rsqrt(jnp.mean(token_f * token_f, axis=-1, keepdims=True) + EPS)
    normed = (token_f * scale * norm_in[...]).astype(BF16)
    eye = lax.broadcasted_iota(jnp.int32, (n_rows, n_rows), 0) == lax.broadcasted_iota(
        jnp.int32, (n_rows, n_rows), 1
    )

    def column(row):
        return jnp.sum(jnp.where(eye, row, 0.0), axis=-1, keepdims=True)

    positions = column(seq_length[...].astype(F32))
    sine, cosine = sin_cos(positions * inverse[...])
    low_half = lax.broadcasted_iota(jnp.int32, (n_rows, DK), 1) < DK // 2
    sine = jnp.where(low_half, -sine, sine)
    score = route_score[...]
    raised = jnp.exp(score - jnp.max(score, axis=0, keepdims=True))
    softmax = raised / jnp.sum(raised, axis=0, keepdims=True)

    top_k = route_expert.shape[0]
    chosen = [column(route_expert[j : j + 1, :].astype(F32)) for j in range(top_k)]
    weights = [column(softmax[j : j + 1, :]) for j in range(top_k)]

    loads[0].wait()
    query = jnp.dot(normed, wq[...], preferred_element_type=F32).astype(BF16).astype(F32)
    loads[1].wait()
    key = jnp.dot(normed, wk[...], preferred_element_type=F32).astype(BF16).astype(F32)
    loads[2].wait()
    value = jnp.dot(normed, wv[...], preferred_element_type=F32).astype(BF16).astype(F32)

    for h in range(heads):
        q = query[:, h * DK : (h + 1) * DK]
        k = key[:, h * DK : (h + 1) * DK]
        v = value[:, h * DV : (h + 1) * DV]
        q = q * cosine + pltpu.roll(q, DK // 2, 1) * sine
        k = (k * cosine + pltpu.roll(k, DK // 2, 1) * sine) * np.float32(DK**-0.5)
        within = jnp.sum(q * k, axis=-1, keepdims=True) * v
        turned = q.T
        for b in range(n_rows):
            if h == 0 and b % per == 0:
                loads[3 + b // per].wait()
            carried[b : b + 1, :] = jnp.sum(
                turned[:, b : b + 1] * state[b, h], axis=0, keepdims=True
            )
        head = jnp.broadcast_to(t * heads + h, (1, 1)).astype(F32)
        decay = 1.0 - jnp.exp2(-2.0 - 2.0 * head)
        retained = decay * carried[...] + within
        centred = retained - jnp.mean(retained, axis=-1, keepdims=True)
        variance = jnp.mean(centred * centred, axis=-1, keepdims=True)
        normal = (
            centred * lax.rsqrt(variance + EPS) * head_gain[:, h * DV : (h + 1) * DV]
        ).astype(BF16)
        if h == 0:
            loads[3 + n_state].wait()
        product = jnp.dot(normal, wo[h * DV : (h + 1) * DV, :], preferred_element_type=F32)
        attended = product if h == 0 else attended + product
    attended = attended.astype(BF16)
    part[...] = attended

    pl.semaphore_wait(barrier, n_tp - 1 + len(cube))

    sends = []
    for d in range(1, n_tp):
        copy = pltpu.make_async_remote_copy(
            src_ref=part,
            dst_ref=part_in.at[d - 1],
            send_sem=tp_send.at[d - 1],
            recv_sem=tp_recv.at[d - 1],
            device_id=to(e, (t + d) % n_tp),
            device_id_type=pl.DeviceIdType.MESH,
        )
        copy.start()
        sends.append(copy)

    for i, peer in enumerate(cube[:-1]):
        signal(round_sem.at[i], peer)
        pl.semaphore_wait(round_sem.at[i], 1)
    for dx in range(1, n_x):
        signal(ready_sem, to(e, ((x + dx) % n_x) * CORES + c))

    total = attended.astype(F32)
    for copy in sends:
        copy.wait_recv()
    for d in range(1, n_tp):
        total = total + part_in[d - 1].astype(F32)
    resid_f = (token_f + total).astype(BF16).astype(F32)
    resid[...] = resid_f
    scale = lax.rsqrt(jnp.mean(resid_f * resid_f, axis=-1, keepdims=True) + EPS)
    mid = (resid_f * scale * norm_mid[...]).astype(BF16)
    for j in range(CORES):
        rows[e, j] = mid[:, j * half : (j + 1) * half]

    def row_copy(d):
        return pltpu.make_async_remote_copy(
            src_ref=rows.at[e, c],
            dst_ref=rows.at[e, c],
            send_sem=row_send.at[d],
            recv_sem=row_recv.at[d],
            device_id=to((e + d) % n_ep, t),
            device_id_type=pl.DeviceIdType.MESH,
        )

    def row_arrival(d):
        origin = (e + n_ep - d) % n_ep
        return pltpu.make_async_remote_copy(
            src_ref=rows.at[origin, c],
            dst_ref=rows.at[origin, c],
            send_sem=row_send.at[d],
            recv_sem=row_recv.at[d],
            device_id=to((e + d) % n_ep, t),
            device_id_type=pl.DeviceIdType.MESH,
        )

    def forward(d, lane):
        origin = (e + n_ep - d) % n_ep
        return pltpu.make_async_remote_copy(
            src_ref=rows.at[origin, lane],
            dst_ref=rows.at[origin, lane],
            send_sem=fwd_send.at[d],
            recv_sem=fwd_recv.at[d],
            device_id=to(e, sibling),
            device_id_type=pl.DeviceIdType.MESH,
        )

    each(1, n_ep, lambda d: row_copy(d).start())

    def relay(d):
        row_arrival(d).wait_recv()
        forward(d, c).start()

    each(1, n_ep, relay)
    each(1, n_ep, lambda d: forward(d, 1 - c).wait_recv())
    for copy in loads[4 + n_state :]:
        copy.wait()

    group = 8 if n_ep % 8 == 0 else n_ep
    span = group * n_rows

    def expert(i):
        block = rows[pl.ds(i * group, group)]
        gate_sum = jnp.zeros((span, gate.shape[0]), F32)
        up_sum = jnp.zeros((span, gate.shape[0]), F32)
        for j in range(CORES):
            piece = block[:, j].reshape(span, half)
            gate_sum += dot_rows(piece, gate[:, j * half : (j + 1) * half])
            up_sum += dot_rows(piece, up[:, j * half : (j + 1) * half])
        hidden[pl.ds(i * span, span), :] = (jax.nn.silu(gate_sum) * up_sum).astype(BF16)

    each(0, n_ep // group, expert)

    def columns(i, j, core):
        start = pl.multiple_of((j * CORES + core) * quarter, quarter)
        return jnp.dot(
            hidden[pl.ds(i * span, span), :],
            down[:, pl.ds(start, quarter)],
            preferred_element_type=F32,
        )

    pair_copies = []
    for j in range(n_x):

        def other(i, j=j):
            pair_out[j, pl.ds(i * group, group)] = (
                columns(i, j, 1 - c).astype(BF16).reshape(group, n_rows, quarter)
            )

        each(0, n_ep // group, other)
        copy = pltpu.make_async_remote_copy(
            src_ref=pair_out.at[j],
            dst_ref=pair_in.at[j],
            send_sem=pair_send.at[j],
            recv_sem=pair_recv.at[j],
            device_id=to(e, sibling),
            device_id_type=pl.DeviceIdType.MESH,
        )
        copy.start()
        pair_copies.append(copy)

    def return_copy(d, dx):
        target = (e + d) % n_ep
        lane = (x + dx) % n_x
        return pltpu.make_async_remote_copy(
            src_ref=share.at[lane, target],
            dst_ref=arrived.at[dx, d],
            send_sem=ret_send.at[dx, d],
            recv_sem=ret_recv.at[dx, d],
            device_id=to(target, lane * CORES + c),
            device_id_type=pl.DeviceIdType.MESH,
        )

    for dx in range(n_x):

        def own(i, dx=dx):
            mine = columns(i, (x + dx) % n_x, c)
            own_sum[dx, pl.ds(i * group, group)] = mine.reshape(group, n_rows, quarter)

        each(0, n_ep // group, own)
    for copy in pair_copies:
        copy.wait_recv()
    pl.semaphore_wait(ready_sem, n_x - 1)
    for dx in [*range(1, n_x), 0]:
        lane = (x + dx) % n_x

        def add(i, dx=dx, lane=lane):
            here = pl.ds(i * group, group)
            share[lane, here] = (own_sum[dx, here] + pair_in[lane, here].astype(F32)).astype(BF16)

        each(0, n_ep // group, add)
        each(0 if dx else 1, n_ep, lambda d, dx=dx: return_copy(d, dx).start())

    def mixing(d):
        expert_index = ((e + n_ep - d) % n_ep) // SPREAD
        wanted = jnp.broadcast_to(expert_index, (1, 1)).astype(F32)
        total = jnp.where(chosen[0] == wanted, weights[0], 0.0)
        for j in range(1, top_k):
            total = total + jnp.where(chosen[j] == wanted, weights[j], 0.0)
        return total

    start = pl.multiple_of(t * quarter, quarter)
    out_sum = resid[:, pl.ds(start, quarter)] + mixing(0) * share[x, e].astype(F32)
    if n_ep <= 8:
        for dx in [0, *range(1, n_x)]:
            for d in range(0 if dx else 1, n_ep):
                return_copy(d, dx).wait_recv()
                out_sum = out_sum + mixing(d) * arrived[dx, d].astype(F32)
    else:
        for dx in range(n_x):

            def gather(d, carry, dx=dx):
                return_copy(d, dx).wait_recv()
                return carry + mixing(d) * arrived[dx, d].astype(F32)

            out_sum = lax.fori_loop(0 if dx else 1, n_ep, gather, out_sum)
    out[...] = out_sum.astype(BF16)

    for copy in sends + pair_copies:
        copy.wait_send()

    def finish(d):
        row_copy(d).wait_send()
        forward(d, c).wait_send()
        return_copy(d, 0).wait_send()

    each(1, n_ep, finish)
    for dx in range(1, n_x):
        each(0, n_ep, lambda d, dx=dx: return_copy(d, dx).wait_send())


def body(
    n_ep,
    n_tp,
    tokens,
    seq_length,
    ret_state,
    norm_in,
    w_query,
    w_key,
    w_value,
    head_gain,
    w_output,
    norm_mid,
    route_expert,
    route_score,
    expert_gate,
    expert_up,
    expert_down,
):
    n_rows, width = tokens.shape
    quarter = width // n_tp
    half = width // CORES
    n_x = n_tp // CORES
    hidden_units = expert_gate.shape[2]
    angle = np.arange(DK, dtype=np.float64) % (DK // 2)
    inverse = jnp.asarray((10000.0 ** (-angle / (DK // 2))).astype(np.float32)[None, :])
    vmem = pl.BlockSpec(memory_space=pltpu.VMEM)
    anywhere = pl.BlockSpec(memory_space=pl.ANY)
    dma = pltpu.SemaphoreType.DMA
    return pl.pallas_call(
        functools.partial(kernel, n_ep, n_tp),
        out_shape=jax.ShapeDtypeStruct((n_rows, quarter), BF16),
        in_specs=[vmem] * 8 + [anywhere] * 8,
        out_specs=vmem,
        scratch_shapes=[
            pltpu.VMEM(ret_state.shape, F32),
            pltpu.VMEM(w_query.shape, BF16),
            pltpu.VMEM(w_key.shape, BF16),
            pltpu.VMEM(w_value.shape, BF16),
            pltpu.VMEM(w_output.shape, BF16),
            pltpu.VMEM((hidden_units, width), BF16),
            pltpu.VMEM((hidden_units, width), BF16),
            pltpu.VMEM(expert_down.shape[1:], BF16),
            pltpu.VMEM((n_rows, DV), F32),
            pltpu.VMEM((n_rows, width), BF16),
            pltpu.VMEM((n_tp - 1, n_rows, width), BF16),
            pltpu.VMEM((n_rows, width), F32),
            pltpu.VMEM((n_ep, CORES, n_rows, half), BF16),
            pltpu.VMEM((n_ep * n_rows, hidden_units), BF16),
            pltpu.VMEM((n_x, n_ep, n_rows, quarter), BF16),
            pltpu.VMEM((n_x, n_ep, n_rows, quarter), BF16),
            pltpu.VMEM((n_x, n_ep, n_rows, quarter), F32),
            pltpu.VMEM((n_x, n_ep, n_rows, quarter), BF16),
            pltpu.VMEM((n_x, n_ep, n_rows, quarter), BF16),
            pltpu.SemaphoreType.REGULAR((n_ep.bit_length(),)),
            pltpu.SemaphoreType.REGULAR,
            dma((12,)),
            dma((n_tp - 1,)),
            dma((n_tp - 1,)),
            dma((n_ep,)),
            dma((n_ep,)),
            dma((n_ep,)),
            dma((n_ep,)),
            dma((n_x,)),
            dma((n_x,)),
            dma((n_x, n_ep)),
            dma((n_x, n_ep)),
        ],
        compiler_params=pltpu.CompilerParams(collective_id=0, has_side_effects=True),
    )(
        tokens,
        seq_length.reshape(1, n_rows),
        inverse,
        norm_in.reshape(1, width),
        head_gain.reshape(1, -1),
        norm_mid.reshape(1, width),
        route_expert.T,
        route_score.T,
        ret_state,
        w_query,
        w_key,
        w_value,
        w_output,
        jnp.swapaxes(expert_gate, 1, 2),
        jnp.swapaxes(expert_up, 1, 2),
        expert_down,
    )


def solution(mesh):
    placed = (
        P("ep", None),
        P("ep"),
        P("ep", "tp", None, None),
        P(),
        P(None, "tp"),
        P(None, "tp"),
        P(None, "tp"),
        P("tp"),
        P("tp", None),
        P(),
        P("ep", None),
        P("ep", None),
        P("ep", None, "tp"),
        P("ep", None, "tp"),
        P("ep", "tp", None),
    )
    step = functools.partial(body, mesh.shape["ep"], mesh.shape["tp"])
    return jax.shard_map(step, mesh=mesh, in_specs=placed, out_specs=P("ep", "tp"), check_vma=False)
```
